32 devices in a mesh: sp: 4 (over z), fs: 2 (over y), tp: 4 (over x, core).
Axes of the slice: x: 2, y: 2, z: 4, core: 2. Of those that a mesh axis runs over, the one named last changes fastest.
Arguments:
- tokens: bfloat16 [2, 3072, 2304], P('fs', 'sp'), may hold values from -6 to 6
- norm_gain: float32 [2304], replicated, may hold values from 0.1 to 1.9
- query_weight: bfloat16 [2304, 2048], P(('sp', 'fs'), 'tp'), may hold values from -6 to 6
- key_weight: bfloat16 [2304, 512], P(('sp', 'fs'), 'tp'), may hold values from -6 to 6
- value_weight: bfloat16 [2304, 512], P(('sp', 'fs'), 'tp'), may hold values from -0.125 to 0.125
- outer_weight: bfloat16 [2304, 2048], P(('sp', 'fs'), 'tp'), may hold values from -0.125 to 0.125
- inner_weight: bfloat16 [2304, 2048], P(('sp', 'fs'), 'tp'), may hold values from -0.125 to 0.125
- signal_weight: bfloat16 [2304, 2048], P(('sp', 'fs'), 'tp'), may hold values from -0.125 to 0.125
- conv_taps: float32 [3, 2048], P(None, 'tp'), may hold values from -3 to 3
- sink_logit: float32 [32], P('tp'), may hold values from -4 to 4
Outputs:
- attn_out: bfloat16 [2, 3072, 2048], P('fs', 'sp', 'tp')
- conv_out: bfloat16 [2, 3072, 2048], P('fs', 'sp', 'tp')
- log_total: float32 [2, 32, 3072], P('fs', 'tp', 'sp')
The draws below stay inside these ranges and needn't reach their ends.
All inputs are finite; a program needn't handle non-finite values.
Results may differ from the reference program's by a relative error of at most 0.014.
The reference program's roundings to bfloat16 on the way (of `normed`, `product` and `rounded`) count: a program that leaves them out, or rounds other values in their place, can miss the bound.
Values may be sent and summed in bfloat16 or wider, within the bound.
A program may use at most 64 MiB of HBM per device.

```python
import math
import jax
import jax.numpy as jnp
from jax import lax

D = 2304
HEAD = 64
QHEADS = 32
KVHEADS = 8
CHANNELS = 2048
WINDOW = 128
SEQS = 2
LEN = 3072


def draw_tokens(key, part):
    base = jax.random.normal(jax.random.fold_in(key, 3), (SEQS, LEN, D), jnp.float32)
    return jnp.clip(base, -6.0, 6.0).astype(jnp.bfloat16)


def projection_pair(key):
    scaling = 1.0 / math.sqrt(D)
    query_base = jax.random.normal(jax.random.fold_in(key, 21), (D, QHEADS * HEAD), jnp.float32) * scaling
    key_base = jax.random.normal(jax.random.fold_in(key, 22), (D, KVHEADS * HEAD), jnp.float32) * scaling
    return (jnp.clip(query_base, -6.0, 6.0), jnp.clip(key_base, -6.0, 6.0))


def draw_query_weight(key, part):
    return projection_pair(key)[0].astype(jnp.bfloat16)


def draw_key_weight(key, part):
    return projection_pair(key)[1].astype(jnp.bfloat16)


def block_scale(own_key, shape, shards, smallest, top_value):
    gain, own = 1.0, jax.random.fold_in(own_key, 6)
    for position, blocks in shards:
        draws = jnp.exp(jax.random.uniform(jax.random.fold_in(own, position), (blocks,), jnp.float32, smallest / len(shards), top_value / len(shards)))
        gain = gain * jnp.repeat(draws, shape[position] // blocks).reshape([-1 if axis == position else 1 for axis in range(len(shape))])
    return gain


def normal_values(own_key, dims, scale, reach, cuts=(), held_as=jnp.bfloat16):
    drawn = scale * jax.random.normal(own_key, dims, jnp.float32)
    if cuts:
        drawn = drawn * block_scale(own_key, dims, cuts, -0.22, 0.18)
    return jnp.clip(drawn, -reach, reach).astype(held_as)


def setup_inputs(seed: int = 0) -> dict:
    splits = jax.random.split(jax.random.key(seed), 11)
    return {
        "tokens": draw_tokens(jax.random.fold_in(splits[10], 71), 0),
        "norm_gain": jnp.clip(1.0 + 0.18 * jax.random.normal(splits[1], (D,), jnp.float32), 0.1, 1.9),
        "query_weight": draw_query_weight(jax.random.fold_in(splits[10], 71), 0),
        "key_weight": draw_key_weight(jax.random.fold_in(splits[10], 71), 0),
        "value_weight": normal_values(splits[4], (D, KVHEADS * HEAD), D ** -0.5, 0.125, ((0, 8), (1, 4))),
        "outer_weight": normal_values(splits[5], (D, CHANNELS), D ** -0.5, 0.125, ((0, 8), (1, 4))),
        "inner_weight": normal_values(splits[6], (D, CHANNELS), D ** -0.5, 0.125, ((0, 8), (1, 4))),
        "signal_weight": normal_values(splits[7], (D, CHANNELS), D ** -0.5, 0.125, ((0, 8), (1, 4))),
        "conv_taps": normal_values(splits[8], (3, CHANNELS), 0.6, 3.0, ((1, 4),), jnp.float32),
        "sink_logit": normal_values(splits[9], (QHEADS,), 1.5, 4.0, ((0, 4),), jnp.float32),
    }


EPSILON = 1e-06

def normalized(tokens, norm_gain):
    values = tokens.astype(jnp.float32)
    scaling = lax.rsqrt(lax.optimization_barrier(jnp.mean(values * values, axis=-1, keepdims=True)) + EPSILON)
    return (values * scaling * norm_gain).astype(jnp.bfloat16)

def banded_attention(queries, key_proj, value_proj, sink_logit):
    seq_length = queries.shape[0]
    group_size = QHEADS // KVHEADS
    block_count = seq_length // WINDOW
    query_blocks = queries.astype(jnp.float32).reshape(block_count, WINDOW, KVHEADS, group_size, HEAD)
    key_rows = jnp.pad(key_proj.astype(jnp.float32), ((WINDOW, WINDOW), (0, 0))).reshape(block_count + 2, WINDOW, KVHEADS, HEAD)
    value_rows = jnp.pad(value_proj.astype(jnp.float32), ((WINDOW, WINDOW), (0, 0))).reshape(block_count + 2, WINDOW, KVHEADS, HEAD)
    key_span = jnp.concatenate([key_rows[:-2], key_rows[1:-1], key_rows[2:]], axis=1)
    value_span = jnp.concatenate([value_rows[:-2], value_rows[1:-1], value_rows[2:]], axis=1)
    scores = jnp.einsum('bqkgd,bskd->bkgqs', query_blocks, key_span) * (1.0 / math.sqrt(HEAD))
    distance = jnp.arange(WINDOW)[:, None] - jnp.arange(3 * WINDOW)[None, :] + WINDOW
    key_pos = WINDOW * jnp.arange(block_count)[:, None] - WINDOW + jnp.arange(3 * WINDOW)[None, :]
    inside = (jnp.abs(distance)[None] <= WINDOW) & ((key_pos >= 0) & (key_pos < seq_length))[:, None, :]
    slopes = jnp.exp2(-8.0 * jnp.arange(1, QHEADS + 1, dtype=jnp.float32) / QHEADS)
    scores = scores - slopes.reshape(KVHEADS, group_size, 1, 1) * jnp.abs(distance).astype(jnp.float32)
    scores = jnp.where(inside[:, None, None], scores, -jnp.inf)
    sink_grid = sink_logit.reshape(KVHEADS, group_size, 1, 1)
    row_peak = jnp.maximum(lax.optimization_barrier(jnp.max(scores, axis=-1, keepdims=True)), sink_grid)
    weights = jnp.exp(scores - row_peak)
    row_total = lax.optimization_barrier(jnp.sum(weights, axis=-1, keepdims=True)) + jnp.exp(sink_grid - row_peak)
    rounded = lax.optimization_barrier(weights.astype(jnp.bfloat16)).astype(jnp.float32)
    weighted = jnp.einsum('bkgqs,bskd->bqkgd', rounded, value_span)
    attended = (weighted / row_total.transpose(0, 3, 1, 2, 4)).astype(jnp.bfloat16).reshape(seq_length, QHEADS * HEAD)
    log_total = (row_peak + jnp.log(row_total))[..., 0].transpose(1, 2, 0, 3).reshape(QHEADS, seq_length)
    return (attended, log_total)

def reference(tokens, norm_gain, query_weight, key_weight, value_weight, outer_weight, inner_weight, signal_weight, conv_taps, sink_logit):

    def one_sequence(rows_in):
        normed = normalized(rows_in, norm_gain)

        def project(weight):
            return jnp.dot(normed, weight, preferred_element_type=jnp.float32).astype(jnp.bfloat16)
        queries = project(query_weight)
        key_proj = project(key_weight)
        value_proj = project(value_weight)
        outer_gate = project(outer_weight)
        inner_gate = project(inner_weight)
        signal = project(signal_weight)
        product = (inner_gate.astype(jnp.float32) * signal.astype(jnp.float32)).astype(jnp.bfloat16)
        padded = jnp.pad(product, ((1, 1), (0, 0))).astype(jnp.float32)
        mixed_conv = conv_taps[0] * padded[:-2] + conv_taps[1] * padded[1:-1] + conv_taps[2] * padded[2:]
        conv_out = (outer_gate.astype(jnp.float32) * mixed_conv).astype(jnp.bfloat16)
        attended, log_total = banded_attention(queries, key_proj, value_proj, sink_logit)
        return (attended, conv_out, log_total)
    attn_out, conv_out, log_total = lax.map(one_sequence, tokens)
    return (attn_out, conv_out, log_total)
```

```python
import math

import functools

import jax
import jax.numpy as jnp
from jax import lax
from jax.experimental import pallas as pl
from jax.experimental.pallas import tpu as pltpu
from jax.sharding import PartitionSpec as P

HEAD = 64
WINDOW = 128


EPSILON = 1e-06


def extended(value, sides, width):
    for axis, dim in sides:
        size, length = (lax.axis_size(axis), value.shape[dim])
        up = [(i, (i + 1) % size) for i in range(size - 1)]
        down = [(j, i) for i, j in up]
        last = lax.slice_in_dim(value, length - width, length, axis=dim)
        initial = lax.slice_in_dim(value, 0, width, axis=dim)
        before = lax.ppermute(last, axis, up)
        after = lax.ppermute(initial, axis, down)
        value = jnp.concatenate([before, value, after], axis=dim)
    return value


def normalized(tokens, norm_gain):
    values = tokens.astype(jnp.float32)
    scaling = lax.rsqrt(jnp.mean(values * values, axis=-1, keepdims=True) + EPSILON)
    return (values * scaling * norm_gain).astype(jnp.bfloat16)


def folding(normed):

    def add_portions(running, portions, offset):
        return tuple(
            (jnp.dot(normed, portion, preferred_element_type=jnp.float32) for portion in portions)
        )

    return add_portions


def empty_sums(normed, weights):
    return tuple((jnp.zeros((normed.shape[0], weight.shape[1]), jnp.float32) for weight in weights))


def rounded(results):
    return tuple((result.astype(jnp.bfloat16) for result in results))


def gate_product(inner_gate, signal):
    return (inner_gate.astype(jnp.float32) * signal.astype(jnp.float32)).astype(jnp.bfloat16)


def send_edges(key_proj, value_proj, product):
    stacked = jnp.concatenate([key_proj, value_proj], axis=1)
    window_rows = extended(stacked, (("sp", 0),), WINDOW)
    conv_rows = extended(product, (("sp", 0),), 1)
    return (window_rows, conv_rows)


def banded_attention(queries, window_rows, sink_logit, slopes, first_pos, seq_length):
    tok_count = queries.shape[0]
    kv_cols = window_rows.shape[1] // 2
    kv_heads = kv_cols // HEAD
    group_size = queries.shape[1] // (HEAD * kv_heads)
    block_count = tok_count // WINDOW
    query_blocks = queries.reshape(block_count, WINDOW, kv_heads, group_size, HEAD)
    key_rows = window_rows[:, :kv_cols].reshape(block_count + 2, WINDOW, kv_heads, HEAD)
    value_rows = window_rows[:, kv_cols:].reshape(block_count + 2, WINDOW, kv_heads, HEAD)
    key_span = jnp.concatenate([key_rows[:-2], key_rows[1:-1], key_rows[2:]], axis=1)
    value_span = jnp.concatenate([value_rows[:-2], value_rows[1:-1], value_rows[2:]], axis=1)
    scores = jnp.einsum(
        "bqkgd,bskd->bkgqs", query_blocks, key_span, preferred_element_type=jnp.float32
    ) * (1.0 / math.sqrt(HEAD))
    distance = jnp.arange(WINDOW)[:, None] - jnp.arange(3 * WINDOW)[None, :] + WINDOW
    key_pos = (
        first_pos
        - WINDOW
        + WINDOW * jnp.arange(block_count)[:, None]
        + jnp.arange(3 * WINDOW)[None, :]
    )
    inside = (jnp.abs(distance)[None] <= WINDOW) & ((key_pos >= 0) & (key_pos < seq_length))[
        :, None, :
    ]
    scores = scores - slopes.reshape(kv_heads, group_size, 1, 1) * jnp.abs(distance).astype(
        jnp.float32
    )
    scores = jnp.where(inside[:, None, None], scores, -jnp.inf)
    sink_grid = sink_logit.reshape(kv_heads, group_size, 1, 1)
    row_peak = jnp.maximum(jnp.max(scores, axis=-1, keepdims=True), sink_grid)
    weights = jnp.exp(scores - row_peak)
    row_total = jnp.sum(weights, axis=-1, keepdims=True) + jnp.exp(sink_grid - row_peak)
    weighted = jnp.einsum(
        "bkgqs,bskd->bqkgd",
        weights.astype(jnp.bfloat16),
        value_span,
        preferred_element_type=jnp.float32,
    )
    attended = (
        (weighted / row_total.transpose(0, 3, 1, 2, 4))
        .astype(jnp.bfloat16)
        .reshape(tok_count, kv_heads * group_size * HEAD)
    )
    log_total = (
        (row_peak + jnp.log(row_total))[..., 0]
        .transpose(1, 2, 0, 3)
        .reshape(kv_heads * group_size, tok_count)
    )
    return (attended, log_total)


def per_device(
    tokens,
    norm_gain,
    query_weight,
    key_weight,
    value_weight,
    outer_weight,
    inner_weight,
    signal_weight,
    conv_taps,
    sink_logit,
):
    normed = normalized(tokens[0], norm_gain)
    add_portions = folding(normed)
    all_sums = add_portions(
        empty_sums(
            normed,
            (query_weight, key_weight, value_weight, outer_weight, inner_weight, signal_weight),
        ),
        (
            lax.all_gather(query_weight, ("sp", "fs"), axis=0, tiled=True),
            lax.all_gather(key_weight, ("sp", "fs"), axis=0, tiled=True),
            lax.all_gather(value_weight, ("sp", "fs"), axis=0, tiled=True),
            lax.all_gather(outer_weight, ("sp", "fs"), axis=0, tiled=True),
            lax.all_gather(inner_weight, ("sp", "fs"), axis=0, tiled=True),
            lax.all_gather(signal_weight, ("sp", "fs"), axis=0, tiled=True),
        ),
        jnp.int32(0),
    )
    queries, key_proj, value_proj, outer_gate, inner_gate, signal = rounded(all_sums)
    product = gate_product(inner_gate, signal)
    window_rows, conv_rows = send_edges(key_proj, value_proj, product)
    tok_count = normed.shape[0]
    head_local = queries.shape[1] // HEAD
    head_index = lax.axis_index("tp") * head_local + jnp.arange(1, head_local + 1)
    slopes = jnp.exp2(-8.0 * head_index.astype(jnp.float32) / (head_local * lax.axis_size("tp")))
    first_pos = lax.axis_index("sp") * tok_count
    attended, log_total = banded_attention(
        queries, window_rows, sink_logit, slopes, first_pos, tok_count * lax.axis_size("sp")
    )
    mixed_conv = conv_taps[0] * conv_rows[0:tok_count].astype(jnp.float32)
    mixed_conv = mixed_conv + conv_taps[1] * conv_rows[1 : tok_count + 1].astype(jnp.float32)
    mixed_conv = mixed_conv + conv_taps[2] * conv_rows[2 : tok_count + 2].astype(jnp.float32)
    conv_out = (outer_gate.astype(jnp.float32) * mixed_conv).astype(jnp.bfloat16)
    return (attended[None], conv_out[None], log_total[None])


MESH = pl.DeviceIdType.MESH
GROUPS = 3
FAR = -1e30


def mega_kernel(
    ns,
    tokens,
    gain,
    qw,
    kvw,
    ow,
    iw,
    sw,
    taps,
    slopes,
    sinks,
    attn_out,
    conv_out,
    log_out,
    toks,
    wts,
    stage_w,
    qs,
    kvs,
    bias,
    prod,
    outer,
    attn_st,
    log_st,
    conv_st,
    load_sem,
    stage_sem,
    misc_sem,
    y_send,
    w_recv,
    up_send,
    dn_send,
    tok_send,
    tok_recv,
    kv_send,
    kv_recv,
    pr_send,
    pr_recv,
    ret_send,
    ret_recv,
):
    s, f, t = lax.axis_index("sp"), lax.axis_index("fs"), lax.axis_index("tp")
    other = 1 - f
    core = lax.rem(t, 2)
    mate = t + 1 - 2 * core
    rows = tokens.shape[0]
    half_rows = rows // 2
    depth = qw.shape[0]
    qcols = qs.shape[2]
    heads = qcols // HEAD
    chans = prod.shape[3]
    blocks = rows // WINDOW
    pad = (prod.shape[2] - rows) // 2
    up, down, across, beside = (s + 1, f, t), (s - 1, f, t), (s, other, t), (s, f, mate)
    has_up, has_down = s < ns - 1, s > 0

    barrier = pltpu.get_barrier_semaphore()

    @pl.when(has_up)
    def _():
        pl.semaphore_signal(barrier, inc=1, device_id=up, device_id_type=MESH)

    @pl.when(has_down)
    def _():
        pl.semaphore_signal(barrier, inc=1, device_id=down, device_id_type=MESH)

    pl.semaphore_signal(barrier, inc=1, device_id=across, device_id_type=MESH)
    pl.semaphore_signal(barrier, inc=1, device_id=beside, device_id_type=MESH)

    def block_rows(blk):
        return pl.ds(pl.multiple_of(blk * depth, 16), depth)

    def loads(g, half, dest, sems):
        if g == 0:
            qc = pl.ds(pl.multiple_of(half * qcols, 128), qcols)
            pairs = [
                (qw.at[:, qc], dest.at[:, pl.ds(0, qcols)]),
                (kvw.at[half], dest.at[:, pl.ds(qcols, 2 * HEAD)]),
            ]
        else:
            c = pl.ds(pl.multiple_of(half * (2 * chans) + (g - 1) * chans, 128), chans)
            pairs = [
                (ref.at[:, c], dest.at[:, pl.ds(i * chans, chans)])
                for i, ref in enumerate((iw, sw, ow))
            ]
        return [
            pltpu.make_async_copy(a, b, sems.at[g, i]) for i, (a, b) in enumerate(pairs)
        ]

    mine = s * 2 + f
    theirs = s * 2 + other
    own_loads = [loads(g, f, wts.at[g, block_rows(mine)], load_sem) for g in range(GROUPS)]
    out_loads = [loads(g, other, stage_w.at[g], stage_sem) for g in range(GROUPS)]
    for g in range(GROUPS):
        for c in out_loads[g] + own_loads[g]:
            c.start()
    tok_load = pltpu.make_async_copy(tokens, toks.at[f], misc_sem.at[0])
    tok_load.start()

    pl.semaphore_wait(
        barrier, 2 + jnp.where(has_up, 1, 0) + jnp.where(has_down, 1, 0)
    )

    y_copies = []
    for g in range(GROUPS):
        for c in out_loads[g]:
            c.wait()
        copy = pltpu.make_async_remote_copy(
            src_ref=stage_w.at[g],
            dst_ref=wts.at[g, block_rows(mine)],
            send_sem=y_send.at[g],
            recv_sem=w_recv.at[g, mine],
            device_id=across,
            device_id_type=MESH,
        )
        copy.start()
        y_copies.append(copy)
        for c in own_loads[g]:
            c.wait()
    share = pl.ds(pl.multiple_of(core * half_rows, 16), half_rows)
    rest = pl.ds(pl.multiple_of((1 - core) * half_rows, 16), half_rows)
    tok_copy = pltpu.make_async_remote_copy(
        src_ref=tokens.at[share],
        dst_ref=toks.at[f, share],
        send_sem=tok_send.at[0],
        recv_sem=tok_recv.at[0],
        device_id=across,
        device_id_type=MESH,
    )
    tok_copy.start()

    def incoming(g, blk):
        return pltpu.make_async_remote_copy(
            src_ref=wts.at[g, block_rows(blk)],
            dst_ref=wts.at[g, block_rows(blk)],
            send_sem=up_send.at[g, blk],
            recv_sem=w_recv.at[g, blk],
            device_id=across,
            device_id_type=MESH,
        )

    def forward(g, blk, upward):
        return pltpu.make_async_remote_copy(
            src_ref=wts.at[g, block_rows(blk)],
            dst_ref=wts.at[g, block_rows(blk)],
            send_sem=(up_send if upward else dn_send).at[g, blk],
            recv_sem=w_recv.at[g, blk],
            device_id=up if upward else down,
            device_id_type=MESH,
        )

    def relay_step(g, d, par):
        side = f if par == 0 else other
        if d == 0:
            blk = s * 2 + side
            if par == 1:
                incoming(g, blk).wait_recv()

            @pl.when(has_up)
            def _():
                forward(g, blk, True).start()

            @pl.when(has_down)
            def _():
                forward(g, blk, False).start()

            return

        @pl.when(s - d >= 0)
        def _():
            blk = (s - d) * 2 + side
            incoming(g, blk).wait_recv()

            @pl.when(has_up)
            def _():
                forward(g, blk, True).start()

        @pl.when(s + d < ns)
        def _():
            blk = (s + d) * 2 + side
            incoming(g, blk).wait_recv()

            @pl.when(has_down)
            def _():
                forward(g, blk, False).start()

    def settle():
        for g in range(GROUPS):
            y_copies[g].wait_send()
            for d in range(ns):
                for par in range(2):
                    side = f if par == 0 else other

                    @pl.when((s - d >= 0) & has_up)
                    def _():
                        forward(g, (s - d) * 2 + side, True).wait_send()

                    @pl.when((s + d < ns) & has_down)
                    def _():
                        forward(g, (s + d) * 2 + side, False).wait_send()

    def norm_rows(seq):
        @pl.loop(0, blocks)
        def _(b):
            at = pl.ds(pl.multiple_of(b * WINDOW, WINDOW), WINDOW)
            values = toks[seq, at, :].astype(jnp.float32)
            scaling = lax.rsqrt(jnp.mean(values * values, axis=-1, keepdims=True) + EPSILON)
            toks[seq, at, :] = (values * scaling * gain[...]).astype(jnp.bfloat16)

    mm_rows = rows // 2

    def make_bias():
        key = lax.broadcasted_iota(jnp.int32, (3 * WINDOW, WINDOW), 0)
        query = lax.broadcasted_iota(jnp.int32, (3 * WINDOW, WINDOW), 1)
        away = jnp.abs(query - key + WINDOW)
        for h in range(heads):
            slope = slopes[f * heads + h]
            bias[h] = jnp.where(away <= WINDOW, -slope * away.astype(jnp.float32), FAR)

    def project_qkv(seq):
        @pl.loop(0, 2)
        def _(b):
            at = pl.multiple_of(b * mm_rows, WINDOW)
            out = jnp.dot(
                toks[seq, pl.ds(at, mm_rows), :], wts[0], preferred_element_type=jnp.float32
            )
            qs[seq, pl.ds(at, mm_rows), :] = out[:, :qcols].astype(jnp.bfloat16)
            kvs[seq, pl.ds(at + WINDOW, mm_rows), :] = out[:, qcols:].astype(jnp.bfloat16)

    def edge_copies(buf, seq, width, sends, recvs, slot):
        length = buf.shape[1] if len(buf.shape) == 3 else buf.shape[2]
        ref = buf.at[seq] if len(buf.shape) == 3 else buf.at[slot // 2, seq]
        climb = pltpu.make_async_remote_copy(
            src_ref=ref.at[pl.ds(length - 2 * width, width)],
            dst_ref=ref.at[pl.ds(0, width)],
            send_sem=sends.at[slot, 0],
            recv_sem=recvs.at[slot, 0],
            device_id=up,
            device_id_type=MESH,
        )
        fall = pltpu.make_async_remote_copy(
            src_ref=ref.at[pl.ds(width, width)],
            dst_ref=ref.at[pl.ds(length - width, width)],
            send_sem=sends.at[slot, 1],
            recv_sem=recvs.at[slot, 1],
            device_id=down,
            device_id_type=MESH,
        )
        return ref, length, climb, fall

    def edges_start(buf, seq, width, sends, recvs, slot):
        ref, length, climb, fall = edge_copies(buf, seq, width, sends, recvs, slot)
        blank = jnp.zeros((width, ref.shape[1]), jnp.bfloat16)

        @pl.when(has_up)
        def _():
            climb.start()

        @pl.when(has_down)
        def _():
            fall.start()

        @pl.when(jnp.logical_not(has_up))
        def _():
            ref[pl.ds(length - width, width), :] = blank

        @pl.when(jnp.logical_not(has_down))
        def _():
            ref[pl.ds(0, width), :] = blank

    def edges_wait(buf, seq, width, sends, recvs, slot):
        _, _, climb, fall = edge_copies(buf, seq, width, sends, recvs, slot)

        @pl.when(has_up)
        def _():
            climb.wait_send()
            fall.wait_recv()

        @pl.when(has_down)
        def _():
            fall.wait_send()
            climb.wait_recv()

    def attend(seq, first, count):
        @pl.loop(first, first + count)
        def _(b):
            at = pl.multiple_of(b * WINDOW, WINDOW)
            kv = kvs[seq, pl.ds(at, 3 * WINDOW), :]
            keys = kv[:, :HEAD]
            values_t = kv.astype(jnp.float32).T[HEAD:, :].astype(jnp.bfloat16)
            queries = qs[seq, pl.ds(at, WINDOW), :]
            low = jnp.where((b == 0) & (s == 0), FAR, 0.0)
            high = jnp.where((b == blocks - 1) & (s == ns - 1), FAR, 0.0)
            outs = []
            for h in range(heads):
                query = queries[:, h * HEAD : (h + 1) * HEAD]
                scores = lax.dot_general(
                    keys, query, (((1,), (1,)), ((), ())), preferred_element_type=jnp.float32
                )
                scores = scores * (1.0 / math.sqrt(HEAD)) + bias[h]
                scores = jnp.concatenate(
                    [
                        scores[:WINDOW] + low,
                        scores[WINDOW : 2 * WINDOW],
                        scores[2 * WINDOW :] + high,
                    ],
                    axis=0,
                )
                sink = sinks[f * heads + h]
                peak = jnp.maximum(jnp.max(scores, axis=0, keepdims=True), sink)
                weights = jnp.exp(scores - peak)
                total = jnp.sum(weights, axis=0, keepdims=True) + jnp.exp(sink - peak)
                mixed = jnp.dot(
                    values_t, weights.astype(jnp.bfloat16), preferred_element_type=jnp.float32
                )
                outs.append(mixed / total)
                log_st[seq, pl.ds(h, 1), pl.ds(at, WINDOW)] = peak + jnp.log(total)
            stacked = jnp.concatenate(outs, axis=0)
            attn_st[seq, pl.ds(at, WINDOW), :] = stacked.T.astype(jnp.bfloat16)

    half_cols = pl.ds(pl.multiple_of(f * qcols, 128), qcols)

    def hand_back(src, dst, slot, seq_is_own):
        if seq_is_own:
            return pltpu.make_async_copy(src, dst, misc_sem.at[1 + slot])
        return pltpu.make_async_remote_copy(
            src_ref=src,
            dst_ref=dst,
            send_sem=ret_send.at[slot],
            recv_sem=ret_recv.at[slot],
            device_id=across,
            device_id_type=MESH,
        )

    def attn_return(own):
        seq = f if own else other
        return [
            hand_back(attn_st.at[seq], attn_out.at[:, half_cols], 0, own),
            hand_back(log_st.at[seq], log_out.at[f], 1, own),
        ]

    def conv_return(g, own):
        seq = f if own else other
        cols = pl.ds(pl.multiple_of(f * (2 * chans) + (g - 1) * chans, 128), chans)
        return [hand_back(conv_st.at[g - 1, seq], conv_out.at[:, cols], 1 + g, own)]

    def project_conv(g, seq):
        @pl.loop(0, 2)
        def _(b):
            at = pl.multiple_of(b * mm_rows, WINDOW)
            out = jnp.dot(
                toks[seq, pl.ds(at, mm_rows), :], wts[g], preferred_element_type=jnp.float32
            )
            inner = out[:, :chans].astype(jnp.bfloat16).astype(jnp.float32)
            signal = out[:, chans : 2 * chans].astype(jnp.bfloat16).astype(jnp.float32)
            prod[g - 1, seq, pl.ds(at + pad, mm_rows), :] = (inner * signal).astype(jnp.bfloat16)
            outer[seq, pl.ds(at, mm_rows), :] = out[:, 2 * chans :].astype(jnp.bfloat16)

    def mix(g, seq):
        cols = pl.ds(pl.multiple_of(f * (2 * chans) + (g - 1) * chans, 128), chans)
        tap = taps[:, cols]
        size = rows + 2 * pad
        full = prod[g - 1, seq].astype(jnp.float32)
        before = pltpu.roll(full, 1, 0)[pad : pad + rows]
        after = pltpu.roll(full, size - 1, 0)[pad : pad + rows]
        mixed = tap[0:1] * before + tap[1:2] * full[pad : pad + rows] + tap[2:3] * after
        conv_st[g - 1, seq] = (outer[seq].astype(jnp.float32) * mixed).astype(jnp.bfloat16)

    def begin(copies):
        for c in copies:
            c.start()

    def pass_tokens():
        return pltpu.make_async_remote_copy(
            src_ref=toks.at[other, share],
            dst_ref=toks.at[other, share],
            send_sem=tok_send.at[1],
            recv_sem=tok_recv.at[1],
            device_id=beside,
            device_id_type=MESH,
        )

    def take_tokens():
        tok_copy.wait_recv()
        pass_tokens().start()

    def ready_tokens():
        pass_tokens().wait_recv()
        pass_tokens().wait_send()
        norm_rows(other)

    def first_own():
        tok_load.wait()
        norm_rows(f)

    def kv_start(seq, slot):
        edges_start(kvs, seq, WINDOW, kv_send, kv_recv, slot)

    def kv_wait(seq, slot):
        edges_wait(kvs, seq, WINDOW, kv_send, kv_recv, slot)

    def pr_start(g, seq, slot):
        edges_start(prod, seq, pad, pr_send, pr_recv, (g - 1) * 2 + slot)

    def pr_wait(g, seq, slot):
        edges_wait(prod, seq, pad, pr_send, pr_recv, (g - 1) * 2 + slot)

    def qkv_own():
        project_qkv(f)
        kv_start(f, 0)

    def qkv_other():
        project_qkv(other)
        kv_start(other, 1)

    def finish_conv(g, own):
        seq, slot = (f, 0) if own else (other, 1)
        pr_wait(g, seq, slot)
        mix(g, seq)
        begin(conv_return(g, own))

    def both_parts(g, own):
        seq, slot = (f, 0) if own else (other, 1)
        project_conv(g, seq)
        pr_start(g, seq, slot)

    third = blocks // 3 if blocks % 3 == 0 else blocks
    parts = blocks // third

    def attend_part(seq, i):
        if i < parts:
            attend(seq, i * third, third)

    plan = {
        (0, 0): [make_bias],
        (0, 2): [first_own],
        (1, 0): [qkv_own],
        (1, 2): [lambda: kv_wait(f, 0), lambda: attend_part(f, 0)],
        (1, 3): [lambda: attend_part(f, 1)],
        (1, 4): [lambda: attend_part(f, 2), lambda: begin(attn_return(True))],
        (1, 7): [take_tokens],
        (2, 0): [lambda: both_parts(1, True)],
        (2, 1): [ready_tokens],
        (2, 2): [qkv_other, lambda: finish_conv(1, True)],
        (2, 3): [lambda: both_parts(1, False)],
        (2, 4): [lambda: kv_wait(other, 1), lambda: attend_part(other, 0)],
        (2, 5): [lambda: attend_part(other, 1)],
        (2, 6): [lambda: attend_part(other, 2), lambda: begin(attn_return(False))],
        (2, 7): [lambda: finish_conv(1, False)],
    }
    spare = dict(plan)
    for g in range(GROUPS):
        for d in range(ns):
            for par in range(2):
                relay_step(g, d, par)
                for piece in spare.pop((g, d * 2 + par), []):
                    piece()
        for key in sorted(k for k in spare if k[0] == g):
            for piece in spare.pop(key):
                piece()

    both_parts(2, False)
    finish_conv(2, False)
    both_parts(2, True)
    finish_conv(2, True)

    tok_copy.wait_send()
    settle()
    for own in (True, False):
        for c in attn_return(own) + conv_return(1, own) + conv_return(2, own):
            c.wait()


def fused_device(
    ns,
    tokens,
    norm_gain,
    query_weight,
    key_weight,
    value_weight,
    outer_weight,
    inner_weight,
    signal_weight,
    conv_taps,
    sink_logit,
):
    rows, width = tokens.shape[1:]
    depth, local = query_weight.shape
    qcols = local // 2
    heads = qcols // HEAD
    chans = outer_weight.shape[1] // 4
    head_local = 2 * heads
    head_index = lax.axis_index("tp") * head_local + jnp.arange(1, head_local + 1)
    slopes = jnp.exp2(-8.0 * head_index.astype(jnp.float32) / (head_local * lax.axis_size("tp")))
    kv_weight = jnp.stack(
        [
            jnp.concatenate([w[:, i * HEAD : (i + 1) * HEAD] for w in (key_weight, value_weight)], 1)
            for i in range(2)
        ]
    )
    group_cols = qcols + 2 * HEAD
    pad = 16
    bf, f32 = jnp.bfloat16, jnp.float32
    dma = pltpu.SemaphoreType.DMA
    hbm = pl.BlockSpec(memory_space=pl.ANY)
    vmem = pl.BlockSpec(memory_space=pltpu.VMEM)
    smem = pl.BlockSpec(memory_space=pltpu.SMEM)
    attended, conv, logs = pl.pallas_call(
        functools.partial(mega_kernel, ns),
        out_shape=(
            jax.ShapeDtypeStruct((rows, local), bf),
            jax.ShapeDtypeStruct((rows, 4 * chans), bf),
            jax.ShapeDtypeStruct((2, heads, rows), f32),
        ),
        in_specs=[hbm, vmem, hbm, hbm, hbm, hbm, hbm, vmem, smem, smem],
        out_specs=(hbm, hbm, hbm),
        scratch_shapes=[
            pltpu.VMEM((2, rows, width), bf),
            pltpu.VMEM((GROUPS, width, group_cols), bf),
            pltpu.VMEM((GROUPS, depth, group_cols), bf),
            pltpu.VMEM((2, rows, qcols), bf),
            pltpu.VMEM((2, rows + 2 * WINDOW, 2 * HEAD), bf),
            pltpu.VMEM((heads, 3 * WINDOW, WINDOW), f32),
            pltpu.VMEM((2, 2, rows + 2 * pad, chans), bf),
            pltpu.VMEM((2, rows, chans), bf),
            pltpu.VMEM((2, rows, qcols), bf),
            pltpu.VMEM((2, heads, rows), f32),
            pltpu.VMEM((2, 2, rows, chans), bf),
            dma((GROUPS, 3)),
            dma((GROUPS, 3)),
            dma((5,)),
            dma((GROUPS,)),
            dma((GROUPS, 2 * ns)),
            dma((GROUPS, 2 * ns)),
            dma((GROUPS, 2 * ns)),
            dma((2,)),
            dma((2,)),
            dma((2, 2)),
            dma((2, 2)),
            dma((4, 2)),
            dma((4, 2)),
            dma((4,)),
            dma((4,)),
        ],
        compiler_params=pltpu.CompilerParams(
            collective_id=0, has_side_effects=True, vmem_limit_bytes=48 << 20
        ),
    )(
        tokens[0],
        norm_gain[None],
        query_weight,
        kv_weight,
        outer_weight,
        inner_weight,
        signal_weight,
        conv_taps,
        slopes,
        sink_logit,
    )
    return (attended[None], conv[None], logs.reshape(1, head_local, rows))


def fits(mesh, args):
    tokens, query_weight, key_weight, outer_weight = (args[i] for i in (0, 2, 3, 5))
    sp, fs, tp = (mesh.shape[a] for a in ("sp", "fs", "tp"))
    rows = tokens.shape[1] // sp
    return (
        fs == 2
        and tokens.shape[0] == fs
        and tp % 2 == 0
        and rows % (2 * WINDOW) == 0
        and key_weight.shape[1] == 2 * HEAD * tp
        and query_weight.shape[1] % (256 * tp) == 0
        and outer_weight.shape[1] == 512 * tp
        and query_weight.shape[1] == 512 * tp
        and query_weight.shape[0] % (16 * sp * fs) == 0
    )


def solution(mesh):
    in_specs = (
        P("fs", "sp", None),
        P(),
        P(("sp", "fs"), "tp"),
        P(("sp", "fs"), "tp"),
        P(("sp", "fs"), "tp"),
        P(("sp", "fs"), "tp"),
        P(("sp", "fs"), "tp"),
        P(("sp", "fs"), "tp"),
        P(None, "tp"),
        P("tp"),
    )
    out_specs = (P("fs", "sp", "tp"), P("fs", "sp", "tp"), P("fs", "tp", "sp"))

    def run(*args):
        body = per_device
        if fits(mesh, args):
            body = functools.partial(fused_device, mesh.shape["sp"])
        return jax.shard_map(
            body, mesh=mesh, in_specs=in_specs, out_specs=out_specs, check_vma=False
        )(*args)

    return run
```

```python
import math

import functools

import jax
import jax.numpy as jnp
from jax import lax
from jax.experimental import pallas as pl
from jax.experimental.pallas import tpu as pltpu
from jax.sharding import PartitionSpec as P

HEAD = 64
WINDOW = 128


EPSILON = 1e-06


def extended(value, sides, width):
    for axis, dim in sides:
        size, length = (lax.axis_size(axis), value.shape[dim])
        up = [(i, (i + 1) % size) for i in range(size - 1)]
        down = [(j, i) for i, j in up]
        last = lax.slice_in_dim(value, length - width, length, axis=dim)
        initial = lax.slice_in_dim(value, 0, width, axis=dim)
        before = lax.ppermute(last, axis, up)
        after = lax.ppermute(initial, axis, down)
        value = jnp.concatenate([before, value, after], axis=dim)
    return value


def normalized(tokens, norm_gain):
    values = tokens.astype(jnp.float32)
    scaling = lax.rsqrt(jnp.mean(values * values, axis=-1, keepdims=True) + EPSILON)
    return (values * scaling * norm_gain).astype(jnp.bfloat16)


def folding(normed):

    def add_portions(running, portions, offset):
        return tuple(
            (jnp.dot(normed, portion, preferred_element_type=jnp.float32) for portion in portions)
        )

    return add_portions


def empty_sums(normed, weights):
    return tuple((jnp.zeros((normed.shape[0], weight.shape[1]), jnp.float32) for weight in weights))


def rounded(results):
    return tuple((result.astype(jnp.bfloat16) for result in results))


def gate_product(inner_gate, signal):
    return (inner_gate.astype(jnp.float32) * signal.astype(jnp.float32)).astype(jnp.bfloat16)


def send_edges(key_proj, value_proj, product):
    stacked = jnp.concatenate([key_proj, value_proj], axis=1)
    window_rows = extended(stacked, (("sp", 0),), WINDOW)
    conv_rows = extended(product, (("sp", 0),), 1)
    return (window_rows, conv_rows)


def banded_attention(queries, window_rows, sink_logit, slopes, first_pos, seq_length):
    tok_count = queries.shape[0]
    kv_cols = window_rows.shape[1] // 2
    kv_heads = kv_cols // HEAD
    group_size = queries.shape[1] // (HEAD * kv_heads)
    block_count = tok_count // WINDOW
    query_blocks = queries.reshape(block_count, WINDOW, kv_heads, group_size, HEAD)
    key_rows = window_rows[:, :kv_cols].reshape(block_count + 2, WINDOW, kv_heads, HEAD)
    value_rows = window_rows[:, kv_cols:].reshape(block_count + 2, WINDOW, kv_heads, HEAD)
    key_span = jnp.concatenate([key_rows[:-2], key_rows[1:-1], key_rows[2:]], axis=1)
    value_span = jnp.concatenate([value_rows[:-2], value_rows[1:-1], value_rows[2:]], axis=1)
    scores = jnp.einsum(
        "bqkgd,bskd->bkgqs", query_blocks, key_span, preferred_element_type=jnp.float32
    ) * (1.0 / math.sqrt(HEAD))
    distance = jnp.arange(WINDOW)[:, None] - jnp.arange(3 * WINDOW)[None, :] + WINDOW
    key_pos = (
        first_pos
        - WINDOW
        + WINDOW * jnp.arange(block_count)[:, None]
        + jnp.arange(3 * WINDOW)[None, :]
    )
    inside = (jnp.abs(distance)[None] <= WINDOW) & ((key_pos >= 0) & (key_pos < seq_length))[
        :, None, :
    ]
    scores = scores - slopes.reshape(kv_heads, group_size, 1, 1) * jnp.abs(distance).astype(
        jnp.float32
    )
    scores = jnp.where(inside[:, None, None], scores, -jnp.inf)
    sink_grid = sink_logit.reshape(kv_heads, group_size, 1, 1)
    row_peak = jnp.maximum(jnp.max(scores, axis=-1, keepdims=True), sink_grid)
    weights = jnp.exp(scores - row_peak)
    row_total = jnp.sum(weights, axis=-1, keepdims=True) + jnp.exp(sink_grid - row_peak)
    weighted = jnp.einsum(
        "bkgqs,bskd->bqkgd",
        weights.astype(jnp.bfloat16),
        value_span,
        preferred_element_type=jnp.float32,
    )
    attended = (
        (weighted / row_total.transpose(0, 3, 1, 2, 4))
        .astype(jnp.bfloat16)
        .reshape(tok_count, kv_heads * group_size * HEAD)
    )
    log_total = (
        (row_peak + jnp.log(row_total))[..., 0]
        .transpose(1, 2, 0, 3)
        .reshape(kv_heads * group_size, tok_count)
    )
    return (attended, log_total)


def per_device(
    tokens,
    norm_gain,
    query_weight,
    key_weight,
    value_weight,
    outer_weight,
    inner_weight,
    signal_weight,
    conv_taps,
    sink_logit,
):
    normed = normalized(tokens[0], norm_gain)
    add_portions = folding(normed)
    all_sums = add_portions(
        empty_sums(
            normed,
            (query_weight, key_weight, value_weight, outer_weight, inner_weight, signal_weight),
        ),
        (
            lax.all_gather(query_weight, ("sp", "fs"), axis=0, tiled=True),
            lax.all_gather(key_weight, ("sp", "fs"), axis=0, tiled=True),
            lax.all_gather(value_weight, ("sp", "fs"), axis=0, tiled=True),
            lax.all_gather(outer_weight, ("sp", "fs"), axis=0, tiled=True),
            lax.all_gather(inner_weight, ("sp", "fs"), axis=0, tiled=True),
            lax.all_gather(signal_weight, ("sp", "fs"), axis=0, tiled=True),
        ),
        jnp.int32(0),
    )
    queries, key_proj, value_proj, outer_gate, inner_gate, signal = rounded(all_sums)
    product = gate_product(inner_gate, signal)
    window_rows, conv_rows = send_edges(key_proj, value_proj, product)
    tok_count = normed.shape[0]
    head_local = queries.shape[1] // HEAD
    head_index = lax.axis_index("tp") * head_local + jnp.arange(1, head_local + 1)
    slopes = jnp.exp2(-8.0 * head_index.astype(jnp.float32) / (head_local * lax.axis_size("tp")))
    first_pos = lax.axis_index("sp") * tok_count
    attended, log_total = banded_attention(
        queries, window_rows, sink_logit, slopes, first_pos, tok_count * lax.axis_size("sp")
    )
    mixed_conv = conv_taps[0] * conv_rows[0:tok_count].astype(jnp.float32)
    mixed_conv = mixed_conv + conv_taps[1] * conv_rows[1 : tok_count + 1].astype(jnp.float32)
    mixed_conv = mixed_conv + conv_taps[2] * conv_rows[2 : tok_count + 2].astype(jnp.float32)
    conv_out = (outer_gate.astype(jnp.float32) * mixed_conv).astype(jnp.bfloat16)
    return (attended[None], conv_out[None], log_total[None])


MESH = pl.DeviceIdType.MESH
GROUPS = 3
FAR = -1e30


def mega_kernel(
    ns,
    tokens,
    gain,
    qw,
    kw,
    vw,
    ow,
    iw,
    sw,
    taps,
    slopes,
    sinks,
    attn_out,
    conv_out,
    log_out,
    toks,
    wts,
    stage_w,
    qs,
    kvs,
    bias,
    prod,
    outer,
    attn_st,
    log_st,
    conv_st,
    load_sem,
    stage_sem,
    misc_sem,
    y_send,
    w_recv,
    up_send,
    dn_send,
    tok_send,
    tok_recv,
    kv_send,
    kv_recv,
    pr_send,
    pr_recv,
    ret_send,
    ret_recv,
):
    s, f, t = lax.axis_index("sp"), lax.axis_index("fs"), lax.axis_index("tp")
    other = 1 - f
    core = lax.rem(t, 2)
    mate = t + 1 - 2 * core
    rows = tokens.shape[0]
    half_rows = rows // 2
    depth = qw.shape[0]
    qcols = qs.shape[2]
    heads = qcols // HEAD
    chans = prod.shape[3]
    blocks = rows // WINDOW
    pad = (prod.shape[2] - rows) // 2
    up, down, across, beside = (s + 1, f, t), (s - 1, f, t), (s, other, t), (s, f, mate)
    has_up, has_down = s < ns - 1, s > 0

    barrier = pltpu.get_barrier_semaphore()

    @pl.when(has_up)
    def _():
        pl.semaphore_signal(barrier, inc=1, device_id=up, device_id_type=MESH)

    @pl.when(has_down)
    def _():
        pl.semaphore_signal(barrier, inc=1, device_id=down, device_id_type=MESH)

    pl.semaphore_signal(barrier, inc=1, device_id=across, device_id_type=MESH)
    pl.semaphore_signal(barrier, inc=1, device_id=beside, device_id_type=MESH)

    def block_rows(blk):
        return pl.ds(pl.multiple_of(blk * depth, 16), depth)

    def loads(g, half, dest, sems):
        if g == 0:
            qc = pl.ds(pl.multiple_of(half * qcols, 128), qcols)
            pairs = [
                (qw.at[:, qc], dest.at[:, pl.ds(0, qcols)]),
            ]
        else:
            c = pl.ds(pl.multiple_of(half * (2 * chans) + (g - 1) * chans, 128), chans)
            pairs = [
                (ref.at[:, c], dest.at[:, pl.ds(i * chans, chans)])
                for i, ref in enumerate((iw, sw, ow))
            ]
        return [
            pltpu.make_async_copy(a, b, sems.at[g, i]) for i, (a, b) in enumerate(pairs)
        ]

    mine = s * 2 + f
    theirs = s * 2 + other
    own_loads = [loads(g, f, wts.at[g, block_rows(mine)], load_sem) for g in range(GROUPS)]
    out_loads = [loads(g, other, stage_w.at[g], stage_sem) for g in range(GROUPS)]
    for g in range(GROUPS):
        for c in out_loads[g] + own_loads[g]:
            c.start()
    tok_load = pltpu.make_async_copy(tokens, toks.at[f], misc_sem.at[0])
    tok_load.start()

    lane = lax.broadcasted_iota(jnp.int32, (depth, 2 * HEAD), 1)
    k_full, v_full = kw[...].astype(jnp.float32), vw[...].astype(jnp.float32)
    low_pair = jnp.where(lane < HEAD, k_full, pltpu.roll(v_full, HEAD, 1))
    high_pair = jnp.where(lane < HEAD, pltpu.roll(k_full, HEAD, 1), v_full)
    first = f == 0
    kv_cols = pl.ds(qcols, 2 * HEAD)
    stage_w[0, :, kv_cols] = jnp.where(first, high_pair, low_pair).astype(jnp.bfloat16)
    wts[0, block_rows(mine), kv_cols] = jnp.where(first, low_pair, high_pair).astype(jnp.bfloat16)

    pl.semaphore_wait(
        barrier, 2 + jnp.where(has_up, 1, 0) + jnp.where(has_down, 1, 0)
    )

    y_copies = []
    for g in range(GROUPS):
        for c in out_loads[g]:
            c.wait()
        copy = pltpu.make_async_remote_copy(
            src_ref=stage_w.at[g],
            dst_ref=wts.at[g, block_rows(mine)],
            send_sem=y_send.at[g],
            recv_sem=w_recv.at[g, mine],
            device_id=across,
            device_id_type=MESH,
        )
        copy.start()
        y_copies.append(copy)
        for c in own_loads[g]:
            c.wait()
    share = pl.ds(pl.multiple_of(core * half_rows, 16), half_rows)
    rest = pl.ds(pl.multiple_of((1 - core) * half_rows, 16), half_rows)
    tok_copy = pltpu.make_async_remote_copy(
        src_ref=tokens.at[share],
        dst_ref=toks.at[f, share],
        send_sem=tok_send.at[0],
        recv_sem=tok_recv.at[0],
        device_id=across,
        device_id_type=MESH,
    )
    tok_copy.start()

    def incoming(g, blk):
        return pltpu.make_async_remote_copy(
            src_ref=wts.at[g, block_rows(blk)],
            dst_ref=wts.at[g, block_rows(blk)],
            send_sem=up_send.at[g, blk],
            recv_sem=w_recv.at[g, blk],
            device_id=across,
            device_id_type=MESH,
        )

    def forward(g, blk, upward):
        return pltpu.make_async_remote_copy(
            src_ref=wts.at[g, block_rows(blk)],
            dst_ref=wts.at[g, block_rows(blk)],
            send_sem=(up_send if upward else dn_send).at[g, blk],
            recv_sem=w_recv.at[g, blk],
            device_id=up if upward else down,
            device_id_type=MESH,
        )

    def relay_step(g, d, par):
        side = f if par == 0 else other
        if d == 0:
            blk = s * 2 + side
            if par == 1:
                incoming(g, blk).wait_recv()

            @pl.when(has_up)
            def _():
                forward(g, blk, True).start()

            @pl.when(has_down)
            def _():
                forward(g, blk, False).start()

            return

        @pl.when(s - d >= 0)
        def _():
            blk = (s - d) * 2 + side
            incoming(g, blk).wait_recv()

            @pl.when(has_up)
            def _():
                forward(g, blk, True).start()

        @pl.when(s + d < ns)
        def _():
            blk = (s + d) * 2 + side
            incoming(g, blk).wait_recv()

            @pl.when(has_down)
            def _():
                forward(g, blk, False).start()

    def settle():
        for g in range(GROUPS):
            y_copies[g].wait_send()
            for d in range(ns):
                for par in range(2):
                    side = f if par == 0 else other

                    @pl.when((s - d >= 0) & has_up)
                    def _():
                        forward(g, (s - d) * 2 + side, True).wait_send()

                    @pl.when((s + d < ns) & has_down)
                    def _():
                        forward(g, (s + d) * 2 + side, False).wait_send()

    def norm_rows(seq):
        @pl.loop(0, blocks)
        def _(b):
            at = pl.ds(pl.multiple_of(b * WINDOW, WINDOW), WINDOW)
            values = toks[seq, at, :].astype(jnp.float32)
            scaling = lax.rsqrt(jnp.mean(values * values, axis=-1, keepdims=True) + EPSILON)
            toks[seq, at, :] = (values * scaling * gain[...]).astype(jnp.bfloat16)

    mm_rows = rows // 2

    def make_bias():
        key = lax.broadcasted_iota(jnp.int32, (3 * WINDOW, WINDOW), 0)
        query = lax.broadcasted_iota(jnp.int32, (3 * WINDOW, WINDOW), 1)
        away = jnp.abs(query - key + WINDOW)
        for h in range(heads):
            slope = slopes[f * heads + h]
            bias[h] = jnp.where(away <= WINDOW, -slope * away.astype(jnp.float32), FAR)

    def project_qkv(seq):
        @pl.loop(0, 2)
        def _(b):
            at = pl.multiple_of(b * mm_rows, WINDOW)
            out = jnp.dot(
                toks[seq, pl.ds(at, mm_rows), :], wts[0], preferred_element_type=jnp.float32
            )
            qs[seq, pl.ds(at, mm_rows), :] = out[:, :qcols].astype(jnp.bfloat16)
            kvs[seq, pl.ds(at + WINDOW, mm_rows), :] = out[:, qcols:].astype(jnp.bfloat16)

    def edge_copies(buf, seq, width, sends, recvs, slot):
        length = buf.shape[1] if len(buf.shape) == 3 else buf.shape[2]
        ref = buf.at[seq] if len(buf.shape) == 3 else buf.at[slot // 2, seq]
        climb = pltpu.make_async_remote_copy(
            src_ref=ref.at[pl.ds(length - 2 * width, width)],
            dst_ref=ref.at[pl.ds(0, width)],
            send_sem=sends.at[slot, 0],
            recv_sem=recvs.at[slot, 0],
            device_id=up,
            device_id_type=MESH,
        )
        fall = pltpu.make_async_remote_copy(
            src_ref=ref.at[pl.ds(width, width)],
            dst_ref=ref.at[pl.ds(length - width, width)],
            send_sem=sends.at[slot, 1],
            recv_sem=recvs.at[slot, 1],
            device_id=down,
            device_id_type=MESH,
        )
        return ref, length, climb, fall

    def edges_start(buf, seq, width, sends, recvs, slot):
        ref, length, climb, fall = edge_copies(buf, seq, width, sends, recvs, slot)
        blank = jnp.zeros((width, ref.shape[1]), jnp.bfloat16)

        @pl.when(has_up)
        def _():
            climb.start()

        @pl.when(has_down)
        def _():
            fall.start()

        @pl.when(jnp.logical_not(has_up))
        def _():
            ref[pl.ds(length - width, width), :] = blank

        @pl.when(jnp.logical_not(has_down))
        def _():
            ref[pl.ds(0, width), :] = blank

    def edges_wait(buf, seq, width, sends, recvs, slot):
        _, _, climb, fall = edge_copies(buf, seq, width, sends, recvs, slot)

        @pl.when(has_up)
        def _():
            climb.wait_send()
            fall.wait_recv()

        @pl.when(has_down)
        def _():
            fall.wait_send()
            climb.wait_recv()

    def attend(seq, first, count):
        @pl.loop(first, first + count)
        def _(b):
            at = pl.multiple_of(b * WINDOW, WINDOW)
            kv = kvs[seq, pl.ds(at, 3 * WINDOW), :]
            keys = kv[:, :HEAD]
            values_t = kv.astype(jnp.float32).T[HEAD:, :].astype(jnp.bfloat16)
            queries = qs[seq, pl.ds(at, WINDOW), :]
            low = jnp.where((b == 0) & (s == 0), FAR, 0.0)
            high = jnp.where((b == blocks - 1) & (s == ns - 1), FAR, 0.0)
            outs = []
            for h in range(heads):
                query = queries[:, h * HEAD : (h + 1) * HEAD]
                scores = lax.dot_general(
                    keys, query, (((1,), (1,)), ((), ())), preferred_element_type=jnp.float32
                )
                scores = scores * (1.0 / math.sqrt(HEAD)) + bias[h]
                scores = jnp.concatenate(
                    [
                        scores[:WINDOW] + low,
                        scores[WINDOW : 2 * WINDOW],
                        scores[2 * WINDOW :] + high,
                    ],
                    axis=0,
                )
                sink = sinks[f * heads + h]
                peak = jnp.maximum(jnp.max(scores, axis=0, keepdims=True), sink)
                weights = jnp.exp(scores - peak)
                total = jnp.sum(weights, axis=0, keepdims=True) + jnp.exp(sink - peak)
                mixed = jnp.dot(
                    values_t, weights.astype(jnp.bfloat16), preferred_element_type=jnp.float32
                )
                outs.append(mixed / total)
                log_st[seq, pl.ds(h, 1), pl.ds(at, WINDOW)] = peak + jnp.log(total)
            stacked = jnp.concatenate(outs, axis=0)
            attn_st[seq, pl.ds(at, WINDOW), :] = stacked.T.astype(jnp.bfloat16)

    half_cols = pl.ds(pl.multiple_of(f * qcols, 128), qcols)

    def hand_back(src, dst, slot, seq_is_own):
        if seq_is_own:
            return pltpu.make_async_copy(src, dst, misc_sem.at[1 + slot])
        return pltpu.make_async_remote_copy(
            src_ref=src,
            dst_ref=dst,
            send_sem=ret_send.at[slot],
            recv_sem=ret_recv.at[slot],
            device_id=across,
            device_id_type=MESH,
        )

    def attn_return(own):
        seq = f if own else other
        return [
            hand_back(attn_st.at[seq], attn_out.at[:, half_cols], 0, own),
            hand_back(log_st.at[seq], log_out.at[f], 1, own),
        ]

    def conv_return(g, own):
        seq = f if own else other
        cols = pl.ds(pl.multiple_of(f * (2 * chans) + (g - 1) * chans, 128), chans)
        return [hand_back(conv_st.at[g - 1, seq], conv_out.at[:, cols], 1 + g, own)]

    def project_conv(g, seq):
        @pl.loop(0, 2)
        def _(b):
            at = pl.multiple_of(b * mm_rows, WINDOW)
            out = jnp.dot(
                toks[seq, pl.ds(at, mm_rows), :], wts[g], preferred_element_type=jnp.float32
            )
            inner = out[:, :chans].astype(jnp.bfloat16).astype(jnp.float32)
            signal = out[:, chans : 2 * chans].astype(jnp.bfloat16).astype(jnp.float32)
            prod[g - 1, seq, pl.ds(at + pad, mm_rows), :] = (inner * signal).astype(jnp.bfloat16)
            outer[seq, pl.ds(at, mm_rows), :] = out[:, 2 * chans :].astype(jnp.bfloat16)

    def mix(g, seq):
        cols = pl.ds(pl.multiple_of(f * (2 * chans) + (g - 1) * chans, 128), chans)
        tap = taps[:, cols]
        size = rows + 2 * pad
        full = prod[g - 1, seq].astype(jnp.float32)
        before = pltpu.roll(full, 1, 0)[pad : pad + rows]
        after = pltpu.roll(full, size - 1, 0)[pad : pad + rows]
        mixed = tap[0:1] * before + tap[1:2] * full[pad : pad + rows] + tap[2:3] * after
        conv_st[g - 1, seq] = (outer[seq].astype(jnp.float32) * mixed).astype(jnp.bfloat16)

    def begin(copies):
        for c in copies:
            c.start()

    def pass_tokens():
        return pltpu.make_async_remote_copy(
            src_ref=toks.at[other, share],
            dst_ref=toks.at[other, share],
            send_sem=tok_send.at[1],
            recv_sem=tok_recv.at[1],
            device_id=beside,
            device_id_type=MESH,
        )

    def take_tokens():
        tok_copy.wait_recv()
        pass_tokens().start()

    def ready_tokens():
        pass_tokens().wait_recv()
        pass_tokens().wait_send()
        norm_rows(other)

    def first_own():
        tok_load.wait()
        norm_rows(f)

    def kv_start(seq, slot):
        edges_start(kvs, seq, WINDOW, kv_send, kv_recv, slot)

    def kv_wait(seq, slot):
        edges_wait(kvs, seq, WINDOW, kv_send, kv_recv, slot)

    def pr_start(g, seq, slot):
        edges_start(prod, seq, pad, pr_send, pr_recv, (g - 1) * 2 + slot)

    def pr_wait(g, seq, slot):
        edges_wait(prod, seq, pad, pr_send, pr_recv, (g - 1) * 2 + slot)

    def qkv_own():
        project_qkv(f)
        kv_start(f, 0)

    def qkv_other():
        project_qkv(other)
        kv_start(other, 1)

    def finish_conv(g, own):
        seq, slot = (f, 0) if own else (other, 1)
        pr_wait(g, seq, slot)
        mix(g, seq)
        begin(conv_return(g, own))

    def both_parts(g, own):
        seq, slot = (f, 0) if own else (other, 1)
        project_conv(g, seq)
        pr_start(g, seq, slot)

    third = blocks // 3 if blocks % 3 == 0 else blocks
    parts = blocks // third

    def attend_part(seq, i):
        if i < parts:
            attend(seq, i * third, third)

    def attend_all(seq, own):
        for i in range(parts):
            attend_part(seq, i)
        begin(attn_return(own))

    start_plan = {(0, 0): [make_bias], (0, 2): [first_own], (1, 1): [qkv_own]}
    end_plan = {
        (1, 2): [lambda: kv_wait(f, 0), lambda: attend_part(f, 0)],
        (1, 3): [lambda: attend_part(f, 1)],
        (1, 4): [lambda: attend_part(f, 2), lambda: begin(attn_return(True))],
        (1, 6): [take_tokens],
        (2, 0): [lambda: both_parts(1, True)],
        (2, 1): [ready_tokens, qkv_other, lambda: both_parts(1, False)],
        (2, 2): [lambda: kv_wait(other, 1), lambda: attend_part(other, 0)],
        (2, 3): [lambda: attend_part(other, 1)],
        (2, 4): [lambda: attend_part(other, 2), lambda: begin(attn_return(False))],
        (2, 5): [lambda: finish_conv(1, False)],
        (2, 6): [lambda: finish_conv(1, True)],
    }
    inner_plan = {
        (1, 5): [lambda: kv_wait(f, 0), lambda: attend_part(f, 0)],
        (2, 1): [
            lambda: attend_part(f, 1),
            lambda: attend_part(f, 2),
            lambda: begin(attn_return(True)),
        ],
        (2, 3): [lambda: both_parts(1, True), take_tokens],
        (2, 5): [
            ready_tokens,
            qkv_other,
            lambda: both_parts(1, False),
            lambda: kv_wait(other, 1),
            lambda: attend_all(other, False),
            lambda: finish_conv(1, False),
            lambda: finish_conv(1, True),
        ],
    }

    def run_all(pieces):
        for piece in pieces:
            piece()

    is_end = (s == 0) | (s == ns - 1)
    for g in range(GROUPS):
        for d in range(ns):
            for par in range(2):
                relay_step(g, d, par)
                key = (g, d * 2 + par)
                run_all(start_plan.get(key, []))
                if key in end_plan:
                    pl.when(is_end)(functools.partial(run_all, end_plan[key]))
                if key in inner_plan:
                    pl.when(jnp.logical_not(is_end))(functools.partial(run_all, inner_plan[key]))

    both_parts(2, False)
    finish_conv(2, False)
    both_parts(2, True)
    finish_conv(2, True)

    tok_copy.wait_send()
    settle()
    for own in (True, False):
        for c in attn_return(own) + conv_return(1, own) + conv_return(2, own):
            c.wait()


def fused_device(
    ns,
    tokens,
    norm_gain,
    query_weight,
    key_weight,
    value_weight,
    outer_weight,
    inner_weight,
    signal_weight,
    conv_taps,
    sink_logit,
):
    rows, width = tokens.shape[1:]
    depth, local = query_weight.shape
    qcols = local // 2
    heads = qcols // HEAD
    chans = outer_weight.shape[1] // 4
    head_local = 2 * heads
    head_index = lax.axis_index("tp") * head_local + jnp.arange(1, head_local + 1)
    slopes = jnp.exp2(-8.0 * head_index.astype(jnp.float32) / (head_local * lax.axis_size("tp")))
    group_cols = qcols + 2 * HEAD
    pad = 16
    bf, f32 = jnp.bfloat16, jnp.float32
    dma = pltpu.SemaphoreType.DMA
    hbm = pl.BlockSpec(memory_space=pl.ANY)
    vmem = pl.BlockSpec(memory_space=pltpu.VMEM)
    smem = pl.BlockSpec(memory_space=pltpu.SMEM)
    attended, conv, logs = pl.pallas_call(
        functools.partial(mega_kernel, ns),
        out_shape=(
            jax.ShapeDtypeStruct((rows, local), bf),
            jax.ShapeDtypeStruct((rows, 4 * chans), bf),
            jax.ShapeDtypeStruct((2, heads, rows), f32),
        ),
        in_specs=[hbm, vmem, hbm, vmem, vmem, hbm, hbm, hbm, vmem, smem, smem],
        out_specs=(hbm, hbm, hbm),
        scratch_shapes=[
            pltpu.VMEM((2, rows, width), bf),
            pltpu.VMEM((GROUPS, width, group_cols), bf),
            pltpu.VMEM((GROUPS, depth, group_cols), bf),
            pltpu.VMEM((2, rows, qcols), bf),
            pltpu.VMEM((2, rows + 2 * WINDOW, 2 * HEAD), bf),
            pltpu.VMEM((heads, 3 * WINDOW, WINDOW), f32),
            pltpu.VMEM((2, 2, rows + 2 * pad, chans), bf),
            pltpu.VMEM((2, rows, chans), bf),
            pltpu.VMEM((2, rows, qcols), bf),
            pltpu.VMEM((2, heads, rows), f32),
            pltpu.VMEM((2, 2, rows, chans), bf),
            dma((GROUPS, 3)),
            dma((GROUPS, 3)),
            dma((5,)),
            dma((GROUPS,)),
            dma((GROUPS, 2 * ns)),
            dma((GROUPS, 2 * ns)),
            dma((GROUPS, 2 * ns)),
            dma((2,)),
            dma((2,)),
            dma((2, 2)),
            dma((2, 2)),
            dma((4, 2)),
            dma((4, 2)),
            dma((4,)),
            dma((4,)),
        ],
        compiler_params=pltpu.CompilerParams(
            collective_id=0, has_side_effects=True, vmem_limit_bytes=63 << 20
        ),
    )(
        tokens[0],
        norm_gain[None],
        query_weight,
        key_weight,
        value_weight,
        outer_weight,
        inner_weight,
        signal_weight,
        conv_taps,
        slopes,
        sink_logit,
    )
    return (attended[None], conv[None], logs.reshape(1, head_local, rows))


def fits(mesh, args):
    tokens, query_weight, key_weight, outer_weight = (args[i] for i in (0, 2, 3, 5))
    sp, fs, tp = (mesh.shape[a] for a in ("sp", "fs", "tp"))
    rows = tokens.shape[1] // sp
    return (
        fs == 2
        and sp == 4
        and tokens.shape[0] == fs
        and tp % 2 == 0
        and rows % (2 * WINDOW) == 0
        and key_weight.shape[1] == 2 * HEAD * tp
        and query_weight.shape[1] % (256 * tp) == 0
        and outer_weight.shape[1] == 512 * tp
        and query_weight.shape[1] == 512 * tp
        and query_weight.shape[0] % (16 * sp * fs) == 0
    )


def solution(mesh):
    in_specs = (
        P("fs", "sp", None),
        P(),
        P(("sp", "fs"), "tp"),
        P(("sp", "fs"), "tp"),
        P(("sp", "fs"), "tp"),
        P(("sp", "fs"), "tp"),
        P(("sp", "fs"), "tp"),
        P(("sp", "fs"), "tp"),
        P(None, "tp"),
        P("tp"),
    )
    out_specs = (P("fs", "sp", "tp"), P("fs", "sp", "tp"), P("fs", "tp", "sp"))

    def run(*args):
        body = per_device
        if fits(mesh, args):
            body = functools.partial(fused_device, mesh.shape["sp"])
        return jax.shard_map(
            body, mesh=mesh, in_specs=in_specs, out_specs=out_specs, check_vma=False
        )(*args)

    return run
```
